32 devices in a mesh: sp: 8 (over z, x), tp: 4 (over y, core).
Axes of the slice: x: 2, y: 2, z: 4, core: 2. Of those that a mesh axis runs over, the one named last changes fastest.
Arguments:
- cotangent: bfloat16 [1024, 2048], P('sp'), may hold values from -6 to 6
- mixer_out: bfloat16 [1024, 2048], P('sp'), may hold values from -6 to 6
- expert_ids: int32 [1024, 2], P('sp'), may hold values from 0 to 7, all different within a row; in each aligned block of 128 rows (0 to 127, 128 to 255, ...) at most 64 rows name the same one
- route_weight: float32 [1024, 2], P('sp'), may hold values from 0.3 to 1.5
- saved_normalized: bfloat16 [1024, 2048], P('sp', 'tp'), may hold values from -6 to 6
- inverse_deviation: float32 [1024], P('sp'), may hold values from 0.3 to 3
- channel_norm_gain: float32 [2048], P('tp'), may hold values from 0.1 to 1.9
- taps: float32 [31, 2048], P(None, 'tp'), may hold values from -1 to 1
- proj_weight: bfloat16 [2048, 2048], P('tp'), may hold values from -0.125 to 0.125
- gate_weight: bfloat16 [8, 2048, 2048], P('sp', None, 'tp'), may hold values from -0.125 to 0.125
- up_weight: bfloat16 [8, 2048, 2048], P('sp', None, 'tp'), may hold values from -0.125 to 0.125
- down_weight: bfloat16 [8, 2048, 2048], P('sp', 'tp'), may hold values from -0.125 to 0.125
Outputs:
- grad_mixer_in: bfloat16 [1024, 2048], P('sp', 'tp')
- grad_proj: float32 [2048, 2048], P('sp', 'tp')
- grad_gate: bfloat16 [8, 2048, 2048], P('sp', None, 'tp')
- grad_up: bfloat16 [8, 2048, 2048], P('sp', None, 'tp')
- grad_down: bfloat16 [8, 2048, 2048], P('sp', 'tp')
The draws below stay inside these ranges and needn't reach their ends.
Inputs may be any that keep to these rules, and one draw needn't show every extreme that they name: `expert_ids`: each row names 2 different experts. Within the rows of one index of sp no expert is named more than 64 times, a bound that some block reaches.
All inputs are finite; a program needn't handle non-finite values.
Results may differ from the reference program's by a relative error of at most 0.02.
Values may be sent and summed in bfloat16 or wider, within the bound.
A program may use at most 64 MiB of HBM per device.

```python
import math
import jax
import jax.numpy as jnp
import numpy as np
from jax import lax

D = 2048
CHANNELS = 2048
EXPERT_FF = 2048
WIDTH = 31
TOPK = 2
TOK_DEV = 128
TOKENS = 1024
EXPERTS = 8
CAP = 64
FFD = 512
N_SP = 8
N_TP = 4


def spiked(drawn, own_key, source, target, blocks, factor):
    def block_of(dim):
        return (jnp.arange(drawn.shape[dim]) // (drawn.shape[dim] // blocks)).reshape((-1,) + (1,) * (drawn.ndim - 1 - dim))

    near = jax.random.permutation(own_key, blocks)[block_of(target)]
    second = (block_of(target) + blocks // 2) % blocks
    return jnp.where((block_of(source) == near) | (block_of(source) == second), factor * drawn, drawn)


def block_scale(rng, extent, split, smallest, high):
    def one(axis_at, blocks):
        draws = jax.random.uniform(jax.random.fold_in(jax.random.fold_in(rng, 6), axis_at), (blocks,), jnp.float32, smallest / len(split), high / len(split))
        return jnp.repeat(jnp.exp(draws), extent[axis_at] // blocks).reshape((-1,) + (1,) * (len(extent) - axis_at - 1))

    loudness = one(*split[0])
    for cut in split[1:]:
        loudness = loudness * one(*cut)
    return loudness


def deal_out(stream_key, own, number, rows, amount, top, reach, skew):
    sequence = jax.random.permutation(stream_key, amount)
    crowded, usual = portions_of(amount, rows * top, reach, skew, True), portions_of(amount, rows * top, reach, skew, False)
    places = jnp.arange(amount)

    def named(lengths, offset_by):
        used = int((lengths > 0).sum())
        fixed = max(1, used // 4)
        shifted = fixed + (places - fixed + offset_by * (used - fixed)) % max(1, amount - fixed)
        return jnp.zeros((amount,), jnp.int32).at[sequence[jnp.where(places < fixed, places, shifted)]].set(jnp.asarray(lengths, jnp.int32))

    lengths = jnp.where(number % 4 == 0, named(crowded, number // 4), named(usual, number - number // 4 - 1))
    mixed = jax.random.permutation(jax.random.fold_in(own, 3), amount)
    donor, taker = mixed[0:amount // 2 * 2:2], mixed[1:amount // 2 * 2:2]
    slack = jnp.minimum(lengths[donor] - 1, reach - lengths[taker]) // 2
    slack = jnp.where((donor == sequence[0]) | (taker == sequence[0]) | (lengths[taker] == 0), 0, jnp.maximum(slack, 0))
    shifted = jax.random.randint(jax.random.fold_in(own, 4), (amount // 2,), 0, 1 << 20) % (slack + 1)
    lengths = lengths.at[donor].add(-shifted).at[taker].add(shifted)
    members = jnp.searchsorted(jnp.cumsum(lengths), jnp.arange(rows * top), side="right").astype(jnp.int32)
    table = members.reshape(top, rows).T
    table = table[jax.random.permutation(jax.random.fold_in(own, 1), rows)]
    offset_by = jax.random.randint(jax.random.fold_in(own, 2), (rows, 1), 0, top)
    return jnp.take_along_axis(table, (jnp.arange(top)[None, :] + offset_by) % top, axis=1)


def portions_of(count, total, limit, lean, full):
    loads = [(1 << 20) // math.isqrt(standing ** lean) + 1 for standing in range(1, count + 1)]
    largest = limit if full else min(limit, max(-(-total // count), total * loads[0] // sum(loads)))
    least = 1 if total - largest >= count - 1 else 0
    holding, surplus = [largest] + [least] * (count - 1), total - largest - least * (count - 1)
    while surplus > 0:
        movable = [i for i in range(1, count) if holding[i] < largest] or [i for i in range(1, count) if holding[i] < limit]
        whole, remaining = sum([loads[i] for i in movable]), surplus
        for i in movable:
            extra = min(limit - holding[i], max(1, remaining * loads[i] // whole), surplus)
            holding[i] = holding[i] + extra
            surplus = surplus - extra
    return np.array(holding)


def gaussian(stream_key, shape, deviation, limit, shards=(), kind=jnp.bfloat16):
    result = jax.random.normal(stream_key, shape, jnp.float32) * deviation
    if len(shards) > 0:
        result = block_scale(stream_key, shape, shards, -0.22, 0.18) * result
    return jnp.clip(result, min=-limit, max=limit).astype(kind)


def heavy_noise(key, extent, width, limit, shards, heavy, held_as=jnp.bfloat16):
    result = width * jax.random.normal(key, extent, jnp.float32)
    if shards:
        result = result * block_scale(key, extent, shards, -0.22, 0.18)
    return jnp.clip(spiked(result, jax.random.fold_in(key, 3), *heavy), -limit, limit).astype(held_as)


def setup_inputs(seed: int = 0) -> dict:
    arg_keys = jax.random.split(jax.random.key(seed), 13)
    cotangent = heavy_noise(arg_keys[0], (TOKENS, D), 1.0, 6.0, ((0, 8),), (0, 1, 8, 2.0))
    mixer_out = gaussian(arg_keys[1], (TOKENS, D), 1.0, 6.0, ((0, 8),))
    expert_ids_keys = jax.random.split(jax.random.fold_in(arg_keys[2], 1), TOKENS // TOK_DEV)
    expert_ids_turns = jax.random.permutation(jax.random.fold_in(arg_keys[2], 3), TOKENS // TOK_DEV)
    expert_ids = jax.vmap(lambda own, number: deal_out(jax.random.fold_in(arg_keys[2], 2), own, number, TOK_DEV, EXPERTS, TOPK, CAP, 1))(expert_ids_keys, expert_ids_turns).reshape((TOKENS, TOPK))
    route_weight = jnp.clip(0.3 + 1.2 * jax.random.uniform(arg_keys[3], (TOKENS, TOPK), jnp.float32) ** block_scale(arg_keys[3], (TOKENS, TOPK), ((0, 8),), -0.2, 0.2), 0.3, 1.5)
    saved_normalized = gaussian(arg_keys[4], (TOKENS, CHANNELS), 1.0, 6.0, ((0, 8), (1, 4)))
    inverse_deviation = jnp.clip(jnp.exp(math.log(3.0) - 2.3025851 * jax.random.uniform(arg_keys[5], (TOKENS,), jnp.float32) ** block_scale(arg_keys[5], (TOKENS,), ((0, 8),), -0.2, 0.2)), 0.3, 3.0)
    channel_norm_gain = jnp.clip(1.0 + 0.18 * jax.random.normal(arg_keys[6], (CHANNELS,), jnp.float32), 0.1, 1.9)
    taps = gaussian(arg_keys[7], (WIDTH, CHANNELS), 0.18, 1.0, ((1, 4),), jnp.float32)
    proj_weight = gaussian(arg_keys[8], (CHANNELS, D), CHANNELS ** -0.5, 0.125, ((0, 4),))
    gate_weight = gaussian(arg_keys[9], (EXPERTS, D, EXPERT_FF), D ** -0.5, 0.125, ((0, 8), (2, 4)))
    up_weight = gaussian(arg_keys[10], (EXPERTS, D, EXPERT_FF), D ** -0.5, 0.125, ((0, 8), (2, 4)))
    down_weight = gaussian(arg_keys[11], (EXPERTS, EXPERT_FF, D), EXPERT_FF ** -0.5, 0.125, ((0, 8), (1, 4)))
    return dict(cotangent=cotangent, mixer_out=mixer_out, expert_ids=expert_ids, route_weight=route_weight, saved_normalized=saved_normalized, inverse_deviation=inverse_deviation, channel_norm_gain=channel_norm_gain, taps=taps, proj_weight=proj_weight, gate_weight=gate_weight, up_weight=up_weight, down_weight=down_weight)


def expert_pass(operands):
    routed_rows, routed_grad, w_first, w_third, w_second = operands
    hidden_gate = jnp.dot(routed_rows, w_first, preferred_element_type=jnp.float32)
    hidden_up = jnp.dot(routed_rows, w_third, preferred_element_type=jnp.float32)
    sigma = jax.nn.sigmoid(hidden_gate)
    swish = hidden_gate * sigma
    activ = (swish * hidden_up).astype(jnp.bfloat16)
    grad_second = jnp.dot(activ.T, routed_grad, preferred_element_type=jnp.float32).astype(jnp.bfloat16)
    grad_activ = jnp.dot(routed_grad, w_second.T, preferred_element_type=jnp.float32)
    grad_gpre = (grad_activ * hidden_up * sigma * (1.0 + hidden_gate * (1.0 - sigma))).astype(jnp.bfloat16)
    grad_upre = (grad_activ * swish).astype(jnp.bfloat16)
    grad_first = jnp.dot(routed_rows.T, grad_gpre, preferred_element_type=jnp.float32).astype(jnp.bfloat16)
    grad_third = jnp.dot(routed_rows.T, grad_upre, preferred_element_type=jnp.float32).astype(jnp.bfloat16)
    slot_count = routed_rows.shape[0]
    model_width = routed_rows.shape[1]
    split_gate = grad_gpre.astype(jnp.float32).reshape(slot_count, N_TP, FFD)
    split_upre = grad_upre.astype(jnp.float32).reshape(slot_count, N_TP, FFD)
    first_split = w_first.astype(jnp.float32).reshape(model_width, N_TP, FFD)
    third_split = w_third.astype(jnp.float32).reshape(model_width, N_TP, FFD)
    partial_value = jnp.einsum('rgf,dgf->grd', split_gate, first_split) + jnp.einsum('rgf,dgf->grd', split_upre, third_split)
    rounded = lax.optimization_barrier(partial_value.astype(jnp.bfloat16))
    slot_grad = jnp.sum(rounded.astype(jnp.float32), axis=0).astype(jnp.bfloat16)
    return grad_first, grad_third, grad_second, slot_grad


def reference(cotangent, mixer_out, expert_ids, route_weight, saved_normalized, inverse_deviation, channel_norm_gain, taps,
              proj_weight, gate_weight, up_weight, down_weight):
    onehot = (expert_ids[:, :, None] == jnp.arange(EXPERTS, dtype=jnp.int32)[None, None, :]).astype(jnp.int32)
    flat_hot = onehot.reshape(N_SP, TOK_DEV * TOPK, EXPERTS)
    ranks = jnp.cumsum(flat_hot, axis=1) - flat_hot
    rank_pair = jnp.sum(ranks * flat_hot, axis=2).reshape(TOKENS, TOPK)
    block_index = (jnp.arange(TOKENS, dtype=jnp.int32) // TOK_DEV)[:, None]
    position = (expert_ids * (N_SP * CAP) + block_index * CAP + rank_pair).reshape(-1).astype(jnp.int32)
    rows_pair = jnp.broadcast_to(mixer_out[:, None, :], (TOKENS, TOPK, D)).reshape(-1, D)
    grad_pair = (route_weight[:, :, None] * cotangent.astype(jnp.float32)[:, None, :]).astype(jnp.bfloat16).reshape(-1, D)
    row_buffer = jnp.zeros((EXPERTS * N_SP * CAP, D), jnp.bfloat16).at[position].set(rows_pair)
    grad_buffer = jnp.zeros((EXPERTS * N_SP * CAP, D), jnp.bfloat16).at[position].set(grad_pair)
    row_buffer = row_buffer.reshape(EXPERTS, N_SP * CAP, D)
    grad_buffer = grad_buffer.reshape(EXPERTS, N_SP * CAP, D)
    grad_gate, grad_up, grad_down, slot_grad = lax.map(
        expert_pass, (row_buffer, grad_buffer, gate_weight, up_weight, down_weight))
    returned = slot_grad.reshape(-1, D)[position].reshape(TOKENS, TOPK, D).astype(jnp.float32)
    mixer_grad = (cotangent.astype(jnp.float32) + jnp.sum(returned, axis=1)).astype(jnp.bfloat16)

    normalized_values = saved_normalized.astype(jnp.float32) * channel_norm_gain[None, :]
    sigma = jax.nn.sigmoid(normalized_values)
    act_conv = (normalized_values * sigma).astype(jnp.bfloat16)
    grad_proj = jnp.dot(mixer_grad.T, act_conv, preferred_element_type=jnp.float32)
    grad_act = jnp.dot(mixer_grad, proj_weight.T, preferred_element_type=jnp.float32)
    norm_output_gradient = grad_act * sigma * (1.0 + normalized_values * (1.0 - sigma)) * channel_norm_gain[None, :]
    normalized_input = saved_normalized.astype(jnp.float32)
    gradient_mean = jnp.mean(norm_output_gradient, axis=1, keepdims=True)
    projected_mean = jnp.mean(norm_output_gradient * normalized_input, axis=1, keepdims=True)
    conv_output_gradient = inverse_deviation[:, None] * (norm_output_gradient - gradient_mean - normalized_input * projected_mean)
    padded = jnp.concatenate([conv_output_gradient, jnp.zeros((WIDTH - 1, CHANNELS), jnp.float32)], axis=0)
    total = jnp.zeros((TOKENS, CHANNELS), jnp.float32)
    for tap_index in range(WIDTH):
        total = total + taps[tap_index][None, :] * padded[tap_index:tap_index + TOKENS]
    return total.astype(jnp.bfloat16), grad_proj, grad_gate, grad_up, grad_down
```

```python
import jax
import jax.numpy as jnp
from jax import lax
from jax.sharding import PartitionSpec as P


def from_behind(value, axis, steps):
    count = lax.axis_size(axis)
    leading, last = (max(0, -steps), min(count, count - steps))
    return lax.ppermute(value, axis, [(source, source + steps) for source in range(leading, last)])


def route_table(expert_ids, route_weight, slot_start, slot_span, capacity, experts):
    onehot = (expert_ids[:, :, None] == jnp.arange(experts, dtype=jnp.int32)[None, None, :]).astype(
        jnp.int32
    )
    flat_hot = onehot.reshape(-1, experts)
    ranks = jnp.cumsum(flat_hot, axis=0) - flat_hot
    rank_pair = jnp.sum(ranks * flat_hot, axis=1).reshape(expert_ids.shape)
    slot_index = expert_ids * capacity + rank_pair
    targets = (
        jnp.arange(experts, dtype=jnp.int32)[:, None] * capacity
        + slot_start
        + jnp.arange(slot_span, dtype=jnp.int32)[None, :]
    ).reshape(-1)
    matched = slot_index[None, :, :] == targets[:, None, None]
    dispatch = jnp.any(matched, axis=2).astype(jnp.bfloat16)
    slot_weight = jnp.sum(jnp.where(matched, route_weight[None, :, :], 0.0), axis=(1, 2))
    return (dispatch, slot_weight)


def shards(
    cotangent,
    mixer_out,
    expert_ids,
    route_weight,
    saved_normalized,
    inverse_deviation,
    channel_norm_gain,
    taps,
    proj_weight,
    gate_weight,
    up_weight,
    down_weight,
):
    experts = lax.axis_size("sp")
    groups = lax.axis_size("tp")
    tok_rows, model_width = cotangent.shape
    capacity = groups * max(1, 4 * tok_rows // (experts * groups))
    slot_span = capacity // groups
    slot_start = lax.axis_index("tp") * slot_span
    dispatch, slot_weight = route_table(
        expert_ids, route_weight, slot_start, slot_span, capacity, experts
    )
    sent_rows = jnp.dot(dispatch, mixer_out, preferred_element_type=jnp.float32).astype(
        jnp.bfloat16
    )
    sent_grad = (
        slot_weight[:, None] * jnp.dot(dispatch, cotangent, preferred_element_type=jnp.float32)
    ).astype(jnp.bfloat16)
    sent_rows = sent_rows.reshape(experts, slot_span, model_width)
    sent_grad = sent_grad.reshape(experts, slot_span, model_width)
    shared_rows = (
        lax.all_to_all(sent_rows, "sp", split_axis=0, concat_axis=0, tiled=True),
        lax.all_to_all(sent_grad, "sp", split_axis=0, concat_axis=0, tiled=True),
    )
    routed_rows, routed_grad = (
        lax.all_gather(shared_rows[0], "tp", axis=1, tiled=True),
        lax.all_gather(shared_rows[1], "tp", axis=1, tiled=True),
    )
    full_table, unused_weight = route_table(
        expert_ids, route_weight, 0, capacity, capacity, experts
    )
    routed_rows = routed_rows.reshape(-1, model_width)
    routed_grad = routed_grad.reshape(-1, model_width)
    w_first = gate_weight[0]
    w_third = up_weight[0]
    w_second = down_weight[0]
    contract_last = (((1,), (1,)), ((), ()))
    contract_first = (((0,), (0,)), ((), ()))
    hidden_gate = jnp.dot(routed_rows, w_first, preferred_element_type=jnp.float32)
    hidden_up = jnp.dot(routed_rows, w_third, preferred_element_type=jnp.float32)
    sigma = jax.nn.sigmoid(hidden_gate)
    swish = hidden_gate * sigma
    activ = (swish * hidden_up).astype(jnp.bfloat16)
    grad_second = lax.dot_general(
        activ, routed_grad, contract_first, preferred_element_type=jnp.float32
    ).astype(jnp.bfloat16)
    grad_activ = lax.dot_general(
        routed_grad, w_second, contract_last, preferred_element_type=jnp.float32
    )
    grad_gpre = (grad_activ * hidden_up * sigma * (1.0 + hidden_gate * (1.0 - sigma))).astype(
        jnp.bfloat16
    )
    grad_upre = (grad_activ * swish).astype(jnp.bfloat16)
    grad_first = lax.dot_general(
        routed_rows, grad_gpre, contract_first, preferred_element_type=jnp.float32
    ).astype(jnp.bfloat16)
    grad_third = lax.dot_general(
        routed_rows, grad_upre, contract_first, preferred_element_type=jnp.float32
    ).astype(jnp.bfloat16)
    partial_value = lax.dot_general(
        grad_gpre, w_first, contract_last, preferred_element_type=jnp.float32
    ) + lax.dot_general(grad_upre, w_third, contract_last, preferred_element_type=jnp.float32)
    share = model_width // groups
    partial_groups = jnp.transpose(
        partial_value.astype(jnp.bfloat16).reshape(-1, groups, share), (1, 0, 2)
    )
    summed = lax.psum_scatter(partial_groups, "tp", scatter_dimension=0, tiled=False)
    home_rows = lax.all_to_all(
        summed.reshape(experts, capacity, share),
        "sp",
        split_axis=0,
        concat_axis=0,
        tiled=True,
    )
    returned = lax.dot_general(
        full_table,
        home_rows.reshape(-1, share),
        contract_first,
        preferred_element_type=jnp.float32,
    )
    own_cotangent = lax.dynamic_slice_in_dim(
        cotangent, lax.axis_index("tp") * share, share, axis=1
    )
    mixer_share = (own_cotangent.astype(jnp.float32) + returned).astype(jnp.bfloat16)
    mixer_grad = lax.all_gather(mixer_share, "tp", axis=1, tiled=True)
    normalized_input = saved_normalized.astype(jnp.float32)
    normalized_values = normalized_input * channel_norm_gain[None, :]
    gate_sig = jax.nn.sigmoid(normalized_values)
    act_conv = (normalized_values * gate_sig).astype(jnp.bfloat16)
    every_act = lax.all_gather(act_conv, "sp", axis=0, tiled=True)
    width_share = model_width // experts
    sent_columns = jnp.stack(
        [mixer_grad[:, i * width_share : (i + 1) * width_share] for i in range(experts)]
    )
    every_grad = lax.all_to_all(
        sent_columns, "sp", split_axis=0, concat_axis=0, tiled=True
    ).reshape(-1, width_share)
    grad_proj = lax.dot_general(
        every_grad, every_act, contract_first, preferred_element_type=jnp.float32
    )
    grad_act = lax.dot_general(
        mixer_grad, proj_weight, contract_last, preferred_element_type=jnp.float32
    )
    norm_output_gradient = (
        grad_act
        * gate_sig
        * (1.0 + normalized_values * (1.0 - gate_sig))
        * channel_norm_gain[None, :]
    )
    reduced_totals = lax.psum(
        (
            jnp.sum(norm_output_gradient, axis=1),
            jnp.sum(norm_output_gradient * normalized_input, axis=1),
        ),
        "tp",
    )
    channel_count = saved_normalized.shape[1] * groups
    conv_output_gradient = inverse_deviation[:, None] * (
        norm_output_gradient
        - reduced_totals[0][:, None] / channel_count
        - normalized_input * (reduced_totals[1][:, None] / channel_count)
    )
    reach = taps.shape[0] - 1
    beyond = from_behind(conv_output_gradient[:reach], "sp", -1)
    extended = jnp.concatenate([conv_output_gradient, beyond], axis=0)
    result = jnp.zeros_like(conv_output_gradient)
    for tap_index in range(taps.shape[0]):
        result = result + taps[tap_index][None, :] * extended[tap_index : tap_index + tok_rows]
    return (
        result.astype(jnp.bfloat16),
        grad_proj,
        grad_first[None],
        grad_third[None],
        grad_second[None],
    )


def solution(mesh):
    return jax.shard_map(
        shards,
        mesh=mesh,
        in_specs=(
            P("sp", None),
            P("sp", None),
            P("sp", None),
            P("sp", None),
            P("sp", "tp"),
            P("sp"),
            P("tp"),
            P(None, "tp"),
            P("tp", None),
            P("sp", None, "tp"),
            P("sp", None, "tp"),
            P("sp", "tp", None),
        ),
        out_specs=(
            P("sp", "tp"),
            P("sp", "tp"),
            P("sp", None, "tp"),
            P("sp", None, "tp"),
            P("sp", "tp", None),
        ),
        check_vma=False,
    )
```

```python
import functools

import jax
import jax.numpy as jnp
from jax import lax
from jax.experimental import pallas as pl
from jax.experimental.pallas import tpu as pltpu
from jax.sharding import PartitionSpec as P


def from_behind(value, axis, steps):
    count = lax.axis_size(axis)
    leading, last = (max(0, -steps), min(count, count - steps))
    return lax.ppermute(value, axis, [(source, source + steps) for source in range(leading, last)])


def route_table(expert_ids, route_weight, slot_start, slot_span, capacity, experts):
    onehot = (expert_ids[:, :, None] == jnp.arange(experts, dtype=jnp.int32)[None, None, :]).astype(
        jnp.int32
    )
    flat_hot = onehot.reshape(-1, experts)
    ranks = jnp.cumsum(flat_hot, axis=0) - flat_hot
    rank_pair = jnp.sum(ranks * flat_hot, axis=1).reshape(expert_ids.shape)
    slot_index = expert_ids * capacity + rank_pair
    targets = (
        jnp.arange(experts, dtype=jnp.int32)[:, None] * capacity
        + slot_start
        + jnp.arange(slot_span, dtype=jnp.int32)[None, :]
    ).reshape(-1)
    matched = slot_index[None, :, :] == targets[:, None, None]
    dispatch = jnp.any(matched, axis=2).astype(jnp.bfloat16)
    slot_weight = jnp.sum(jnp.where(matched, route_weight[None, :, :], 0.0), axis=(1, 2))
    return (dispatch, slot_weight)


def remote(source, target, send_sem, recv_sem, device):
    return pltpu.make_async_remote_copy(
        src_ref=source,
        dst_ref=target,
        send_sem=send_sem,
        recv_sem=recv_sem,
        device_id=device,
        device_id_type=pl.DeviceIdType.MESH,
    )


def dispatch_kernel(experts, groups, *refs):
    sent = refs[:2]
    held = refs[2:4]
    local_sem, far_send, far_recv, row_send, row_recv, pair_send, pair_recv = refs[4:]
    mine = lax.axis_index("sp")
    place = lax.axis_index("tp")
    chips = groups // 2
    chip, core = place // 2, place % 2
    sibling = chip * 2 + 1 - core

    def at_chip(step):
        return ((chip + step) % chips) * 2 + core

    barrier = pltpu.get_barrier_semaphore()

    def greet(step, carry):
        pl.semaphore_signal(barrier, inc=1, device_id=((mine + step) % experts, place),
                            device_id_type=pl.DeviceIdType.MESH)
        return carry

    lax.fori_loop(1, experts, greet, 0)
    for step in range(1, chips):
        pl.semaphore_signal(barrier, inc=1, device_id=(mine, at_chip(step)),
                            device_id_type=pl.DeviceIdType.MESH)
    pl.semaphore_signal(barrier, inc=1, device_id=(mine, sibling),
                        device_id_type=pl.DeviceIdType.MESH)
    pl.semaphore_wait(barrier, experts - 1 + chips)

    def far(a, step):
        peer = (mine + step) % experts
        return remote(sent[a].at[peer], held[a].at[mine, place],
                      far_send.at[a, step], far_recv.at[a, step], (peer, place))

    def row(a, step, hop):
        source = (mine + experts - step) % experts
        block = held[a].at[source, place]
        return remote(block, block, row_send.at[a, step, hop], row_recv.at[a, step, hop],
                      (mine, at_chip(hop)))

    def pair(a, step, hop):
        source = (mine + experts - step) % experts
        block = held[a].at[source, at_chip(chips - hop)]
        return remote(block, block, pair_send.at[a, step, hop], pair_recv.at[a, step, hop],
                      (mine, sibling))

    own = [
        pltpu.make_async_copy(sent[a].at[mine], held[a].at[mine, place], local_sem.at[a])
        for a in range(2)
    ]
    for a in range(2):
        own[a].start()
    for a in range(2):
        def start_far(step, carry, a=a):
            far(a, step).start()
            return carry

        lax.fori_loop(1, experts, start_far, 0)

    def pass_on(a, step):
        for hop in range(1, chips):
            row(a, step, hop).start()
        pair(a, step, 0).start()

    def pass_rows(a, step):
        for hop in range(1, chips):
            row(a, step, hop).wait_recv()
            pair(a, step, hop).start()

    for a in range(2):
        own[a].wait()
        pass_on(a, 0)
    for a in range(2):
        def arrive(step, carry, a=a):
            far(a, step).wait_recv()
            pass_on(a, step)
            pass_rows(a, step - 1)
            return carry

        lax.fori_loop(1, experts, arrive, 0)
        pass_rows(a, experts - 1)
    for a in range(2):
        def finish(step, carry, a=a):
            for hop in range(chips):
                pair(a, step, hop).wait()
                if hop:
                    row(a, step, hop).wait_send()
            return carry

        lax.fori_loop(0, experts, finish, 0)

        def finish_far(step, carry, a=a):
            far(a, step).wait_send()
            return carry

        lax.fori_loop(1, experts, finish_far, 0)


def dispatch_blocks(rows, grads, groups):
    experts, span, width = rows.shape
    chips = groups // 2
    full = jax.ShapeDtypeStruct((experts, groups, span, width), rows.dtype)
    dma = pltpu.SemaphoreType.DMA
    return pl.pallas_call(
        functools.partial(dispatch_kernel, experts, groups),
        out_shape=(full, full),
        in_specs=[pl.BlockSpec(memory_space=pltpu.VMEM)] * 2,
        out_specs=[pl.BlockSpec(memory_space=pltpu.VMEM)] * 2,
        scratch_shapes=[dma((2,))]
        + [dma((2, experts))] * 2
        + [dma((2, experts, chips))] * 4,
        compiler_params=pltpu.CompilerParams(
            collective_id=0, has_side_effects=True, vmem_limit_bytes=24 * 2**20
        ),
        cost_estimate=pl.CostEstimate(
            flops=0, bytes_accessed=40 * full.size, transcendentals=0
        ),
    )(rows, grads)


def shards(
    cotangent,
    mixer_out,
    expert_ids,
    route_weight,
    saved_normalized,
    inverse_deviation,
    channel_norm_gain,
    taps,
    proj_weight,
    gate_weight,
    up_weight,
    down_weight,
):
    experts = lax.axis_size("sp")
    groups = lax.axis_size("tp")
    tok_rows, model_width = cotangent.shape
    capacity = groups * max(1, 4 * tok_rows // (experts * groups))
    slot_span = capacity // groups
    slot_start = lax.axis_index("tp") * slot_span
    dispatch, slot_weight = route_table(
        expert_ids, route_weight, slot_start, slot_span, capacity, experts
    )
    sent_rows = jnp.dot(dispatch, mixer_out, preferred_element_type=jnp.float32).astype(
        jnp.bfloat16
    )
    sent_grad = (
        slot_weight[:, None] * jnp.dot(dispatch, cotangent, preferred_element_type=jnp.float32)
    ).astype(jnp.bfloat16)
    sent_rows = sent_rows.reshape(experts, slot_span, model_width)
    sent_grad = sent_grad.reshape(experts, slot_span, model_width)
    normalized_input = saved_normalized.astype(jnp.float32)
    normalized_values = normalized_input * channel_norm_gain[None, :]
    gate_sig = jax.nn.sigmoid(normalized_values)
    act_conv = (normalized_values * gate_sig).astype(jnp.bfloat16)
    act_conv, sent_rows = lax.optimization_barrier((act_conv, sent_rows))
    every_act = lax.all_gather(act_conv, "sp", axis=0, tiled=True)
    routed_rows, routed_grad = dispatch_blocks(sent_rows, sent_grad, groups)
    full_table, unused_weight = route_table(
        expert_ids, route_weight, 0, capacity, capacity, experts
    )
    routed_rows = routed_rows.reshape(-1, model_width)
    routed_grad = routed_grad.reshape(-1, model_width)
    w_first = gate_weight[0]
    w_third = up_weight[0]
    w_second = down_weight[0]
    contract_last = (((1,), (1,)), ((), ()))
    contract_first = (((0,), (0,)), ((), ()))
    hidden_gate = jnp.dot(routed_rows, w_first, preferred_element_type=jnp.float32)
    hidden_up = jnp.dot(routed_rows, w_third, preferred_element_type=jnp.float32)
    sigma = jax.nn.sigmoid(hidden_gate)
    swish = hidden_gate * sigma
    activ = (swish * hidden_up).astype(jnp.bfloat16)
    grad_second = lax.dot_general(
        activ, routed_grad, contract_first, preferred_element_type=jnp.float32
    ).astype(jnp.bfloat16)
    grad_activ = lax.dot_general(
        routed_grad, w_second, contract_last, preferred_element_type=jnp.float32
    )
    grad_gpre = (grad_activ * hidden_up * sigma * (1.0 + hidden_gate * (1.0 - sigma))).astype(
        jnp.bfloat16
    )
    grad_upre = (grad_activ * swish).astype(jnp.bfloat16)
    grad_first = lax.dot_general(
        routed_rows, grad_gpre, contract_first, preferred_element_type=jnp.float32
    ).astype(jnp.bfloat16)
    grad_third = lax.dot_general(
        routed_rows, grad_upre, contract_first, preferred_element_type=jnp.float32
    ).astype(jnp.bfloat16)
    partial_value = lax.dot_general(
        grad_gpre, w_first, contract_last, preferred_element_type=jnp.float32
    ) + lax.dot_general(grad_upre, w_third, contract_last, preferred_element_type=jnp.float32)
    share = model_width // groups
    partial_groups = jnp.transpose(
        partial_value.astype(jnp.bfloat16).reshape(-1, groups, share), (1, 0, 2)
    )
    every_act, partial_groups = lax.optimization_barrier((every_act, partial_groups))
    summed = lax.psum_scatter(partial_groups, "tp", scatter_dimension=0, tiled=False)
    home_rows = lax.all_to_all(
        summed.reshape(experts, capacity, share),
        "sp",
        split_axis=0,
        concat_axis=0,
        tiled=True,
    )
    returned = lax.dot_general(
        full_table,
        home_rows.reshape(-1, share),
        contract_first,
        preferred_element_type=jnp.float32,
    )
    own_cotangent = lax.dynamic_slice_in_dim(
        cotangent, lax.axis_index("tp") * share, share, axis=1
    )
    mixer_share = (own_cotangent.astype(jnp.float32) + returned).astype(jnp.bfloat16)
    mixer_grad = lax.all_gather(mixer_share, "tp", axis=1, tiled=True)
    width_share = model_width // experts
    sent_columns = jnp.transpose(
        mixer_grad.reshape(tok_rows, experts, width_share), (1, 0, 2)
    )
    every_grad = lax.all_to_all(
        sent_columns, "sp", split_axis=0, concat_axis=0, tiled=True
    ).reshape(-1, width_share)
    grad_proj = lax.dot_general(
        every_grad, every_act, contract_first, preferred_element_type=jnp.float32
    )
    grad_act = lax.dot_general(
        mixer_grad, proj_weight, contract_last, preferred_element_type=jnp.float32
    )
    norm_output_gradient = (
        grad_act
        * gate_sig
        * (1.0 + normalized_values * (1.0 - gate_sig))
        * channel_norm_gain[None, :]
    )
    reduced_totals = lax.psum(
        (
            jnp.sum(norm_output_gradient, axis=1),
            jnp.sum(norm_output_gradient * normalized_input, axis=1),
        ),
        "tp",
    )
    channel_count = saved_normalized.shape[1] * groups
    conv_output_gradient = inverse_deviation[:, None] * (
        norm_output_gradient
        - reduced_totals[0][:, None] / channel_count
        - normalized_input * (reduced_totals[1][:, None] / channel_count)
    )
    reach = taps.shape[0] - 1
    beyond = from_behind(conv_output_gradient[:reach], "sp", -1)
    extended = jnp.concatenate([conv_output_gradient, beyond], axis=0)
    result = jnp.zeros_like(conv_output_gradient)
    for tap_index in range(taps.shape[0]):
        result = result + taps[tap_index][None, :] * extended[tap_index : tap_index + tok_rows]
    return (
        result.astype(jnp.bfloat16),
        grad_proj,
        grad_first[None],
        grad_third[None],
        grad_second[None],
    )


def solution(mesh):
    return jax.shard_map(
        shards,
        mesh=mesh,
        in_specs=(
            P("sp", None),
            P("sp", None),
            P("sp", None),
            P("sp", None),
            P("sp", "tp"),
            P("sp"),
            P("tp"),
            P(None, "tp"),
            P("tp", None),
            P("sp", None, "tp"),
            P("sp", None, "tp"),
            P("sp", "tp", None),
        ),
        out_specs=(
            P("sp", "tp"),
            P("sp", "tp"),
            P("sp", None, "tp"),
            P("sp", None, "tp"),
            P("sp", "tp", None),
        ),
        check_vma=False,
    )
```

```python
import functools

import jax
import jax.numpy as jnp
from jax import lax
from jax.experimental import pallas as pl
from jax.experimental.pallas import tpu as pltpu
from jax.sharding import PartitionSpec as P


def from_behind(value, axis, steps):
    count = lax.axis_size(axis)
    leading, last = (max(0, -steps), min(count, count - steps))
    return lax.ppermute(value, axis, [(source, source + steps) for source in range(leading, last)])


def route_table(expert_ids, route_weight, slot_start, slot_span, capacity, experts):
    onehot = (expert_ids[:, :, None] == jnp.arange(experts, dtype=jnp.int32)[None, None, :]).astype(
        jnp.int32
    )
    flat_hot = onehot.reshape(-1, experts)
    ranks = jnp.cumsum(flat_hot, axis=0) - flat_hot
    rank_pair = jnp.sum(ranks * flat_hot, axis=1).reshape(expert_ids.shape)
    slot_index = expert_ids * capacity + rank_pair
    targets = (
        jnp.arange(experts, dtype=jnp.int32)[:, None] * capacity
        + slot_start
        + jnp.arange(slot_span, dtype=jnp.int32)[None, :]
    ).reshape(-1)
    matched = slot_index[None, :, :] == targets[:, None, None]
    dispatch = jnp.any(matched, axis=2).astype(jnp.bfloat16)
    slot_weight = jnp.sum(jnp.where(matched, route_weight[None, :, :], 0.0), axis=(1, 2))
    return (dispatch, slot_weight)


def remote(source, target, send_sem, recv_sem, device):
    return pltpu.make_async_remote_copy(
        src_ref=source,
        dst_ref=target,
        send_sem=send_sem,
        recv_sem=recv_sem,
        device_id=device,
        device_id_type=pl.DeviceIdType.MESH,
    )


def dispatch_kernel(experts, groups, *refs):
    sent = refs[:2]
    held = refs[2:4]
    local_sem, far_send, far_recv, row_send, row_recv, pair_send, pair_recv = refs[4:]
    mine = lax.axis_index("sp")
    place = lax.axis_index("tp")
    chips = groups // 2
    chip, core = place // 2, place % 2
    sibling = chip * 2 + 1 - core

    def at_chip(step):
        return ((chip + step) % chips) * 2 + core

    barrier = pltpu.get_barrier_semaphore()

    def greet(step, carry):
        pl.semaphore_signal(barrier, inc=1, device_id=((mine + step) % experts, place),
                            device_id_type=pl.DeviceIdType.MESH)
        return carry

    lax.fori_loop(1, experts, greet, 0)
    for step in range(1, chips):
        pl.semaphore_signal(barrier, inc=1, device_id=(mine, at_chip(step)),
                            device_id_type=pl.DeviceIdType.MESH)
    pl.semaphore_signal(barrier, inc=1, device_id=(mine, sibling),
                        device_id_type=pl.DeviceIdType.MESH)
    pl.semaphore_wait(barrier, experts - 1 + chips)

    def far(a, step):
        peer = (mine + step) % experts
        return remote(sent[a].at[peer], held[a].at[mine, place],
                      far_send.at[a, step], far_recv.at[a, step], (peer, place))

    def row(a, step, hop):
        source = (mine + experts - step) % experts
        block = held[a].at[source, place]
        return remote(block, block, row_send.at[a, step, hop], row_recv.at[a, step, hop],
                      (mine, at_chip(hop)))

    def pair(a, step, hop):
        source = (mine + experts - step) % experts
        block = held[a].at[source, at_chip(chips - hop)]
        return remote(block, block, pair_send.at[a, step, hop], pair_recv.at[a, step, hop],
                      (mine, sibling))

    own = [
        pltpu.make_async_copy(sent[a].at[mine], held[a].at[mine, place], local_sem.at[a])
        for a in range(2)
    ]
    for a in range(2):
        own[a].start()
    for a in range(2):
        def start_far(step, carry, a=a):
            far(a, step).start()
            return carry

        lax.fori_loop(1, experts, start_far, 0)

    def pass_on(a, step):
        for hop in range(1, chips):
            row(a, step, hop).start()
        pair(a, step, 0).start()

    def pass_rows(a, step):
        for hop in range(1, chips):
            row(a, step, hop).wait_recv()
            pair(a, step, hop).start()

    for a in range(2):
        own[a].wait()
        pass_on(a, 0)
    for a in range(2):
        def arrive(step, carry, a=a):
            far(a, step).wait_recv()
            pass_on(a, step)
            pass_rows(a, step - 1)
            return carry

        lax.fori_loop(1, experts, arrive, 0)
        pass_rows(a, experts - 1)
    for a in range(2):
        def finish(step, carry, a=a):
            for hop in range(chips):
                pair(a, step, hop).wait()
                if hop:
                    row(a, step, hop).wait_send()
            return carry

        lax.fori_loop(0, experts, finish, 0)

        def finish_far(step, carry, a=a):
            far(a, step).wait_send()
            return carry

        lax.fori_loop(1, experts, finish_far, 0)


def dispatch_blocks(rows, grads, groups):
    experts, span, width = rows.shape
    chips = groups // 2
    full = jax.ShapeDtypeStruct((experts, groups, span, width), rows.dtype)
    dma = pltpu.SemaphoreType.DMA
    return pl.pallas_call(
        functools.partial(dispatch_kernel, experts, groups),
        out_shape=(full, full),
        in_specs=[pl.BlockSpec(memory_space=pltpu.VMEM)] * 2,
        out_specs=[pl.BlockSpec(memory_space=pltpu.VMEM)] * 2,
        scratch_shapes=[dma((2,))]
        + [dma((2, experts))] * 2
        + [dma((2, experts, chips))] * 4,
        compiler_params=pltpu.CompilerParams(
            collective_id=0, has_side_effects=True, vmem_limit_bytes=24 * 2**20
        ),
        cost_estimate=pl.CostEstimate(
            flops=0, bytes_accessed=40 * full.size, transcendentals=0
        ),
    )(rows, grads)


def home_kernel(experts, groups, partial, home, pair_in, row_out, row_in, total, *sems):
    pair_send, pair_recv, row_send, row_recv, far_send, far_recv = sems
    mine = lax.axis_index("sp")
    place = lax.axis_index("tp")
    chips = groups // 2
    chip, core = place // 2, place % 2
    sibling = chip * 2 + 1 - core

    def at_chip(step):
        return ((chip + step) % chips) * 2 + core

    barrier = pltpu.get_barrier_semaphore()

    def greet(step, carry):
        pl.semaphore_signal(barrier, inc=1, device_id=((mine + step) % experts, place),
                            device_id_type=pl.DeviceIdType.MESH)
        return carry

    lax.fori_loop(1, experts, greet, 0)
    for step in range(1, chips):
        pl.semaphore_signal(barrier, inc=1, device_id=(mine, at_chip(step)),
                            device_id_type=pl.DeviceIdType.MESH)
    pl.semaphore_signal(barrier, inc=1, device_id=(mine, sibling),
                        device_id_type=pl.DeviceIdType.MESH)
    pl.semaphore_wait(barrier, experts - 1 + chips)

    def pair(step, hop):
        owner = (mine + step + 1) % experts
        other = ((chip + hop) % chips) * 2 + 1 - core
        return remote(partial.at[other, owner], pair_in.at[hop, owner],
                      pair_send.at[step, hop], pair_recv.at[step, hop], (mine, sibling))

    def row(step, hop):
        owner = (mine + step + 1) % experts
        return remote(row_out.at[hop, owner], row_in.at[hop, owner],
                      row_send.at[step, hop], row_recv.at[step, hop], (mine, at_chip(hop)))

    def far(step):
        owner = (mine + step + 1) % experts
        return remote(total.at[owner], home.at[mine],
                      far_send.at[step], far_recv.at[step], (owner, place))

    def start_pair(step, carry):
        for hop in reversed(range(chips)):
            pair(step, hop).start()
        return carry

    lax.fori_loop(0, experts, start_pair, 0)

    def add_pair(step, hop):
        owner = (mine + step + 1) % experts
        pair(step, hop).wait_recv()
        return partial[at_chip(hop), owner].astype(jnp.float32) + pair_in[hop, owner].astype(
            jnp.float32
        )

    def send_rows(step):
        owner = (mine + step + 1) % experts
        for hop in range(1, chips):
            row_out[hop, owner] = add_pair(step, hop).astype(row_out.dtype)
            row(step, hop).start()

    def add_rows(step):
        owner = (mine + step + 1) % experts
        value = add_pair(step, 0)
        for hop in range(1, chips):
            row(step, hop).wait_recv()
            value = value + row_in[hop, owner].astype(jnp.float32)
        return value.astype(total.dtype)

    def advance(step, carry):
        send_rows(step)
        before = step - 1
        total[(mine + before + 1) % experts] = add_rows(before)
        far(before).start()
        return carry

    send_rows(0)
    lax.fori_loop(1, experts, advance, 0)
    home[mine] = add_rows(experts - 1)

    def finish(step, carry):
        for hop in range(chips):
            pair(step, hop).wait_send()
            if hop:
                row(step, hop).wait_send()
        return carry

    lax.fori_loop(0, experts, finish, 0)

    def finish_far(step, carry):
        far(step).wait()
        return carry

    lax.fori_loop(0, experts - 1, finish_far, 0)


def home_blocks(partial):
    groups, experts, capacity, share = partial.shape
    chips = groups // 2
    dma = pltpu.SemaphoreType.DMA
    blocks = pltpu.VMEM((chips, experts, capacity, share), partial.dtype)
    return pl.pallas_call(
        functools.partial(home_kernel, experts, groups),
        out_shape=jax.ShapeDtypeStruct((experts, capacity, share), partial.dtype),
        in_specs=[pl.BlockSpec(memory_space=pltpu.VMEM)],
        out_specs=pl.BlockSpec(memory_space=pltpu.VMEM),
        scratch_shapes=[blocks] * 3
        + [pltpu.VMEM((experts, capacity, share), partial.dtype)]
        + [dma((experts, chips))] * 4
        + [dma((experts,))] * 2,
        compiler_params=pltpu.CompilerParams(
            collective_id=1, has_side_effects=True, vmem_limit_bytes=24 * 2**20
        ),
        cost_estimate=pl.CostEstimate(
            flops=0, bytes_accessed=40 * partial.size, transcendentals=0
        ),
    )(partial)


def shards(
    cotangent,
    mixer_out,
    expert_ids,
    route_weight,
    saved_normalized,
    inverse_deviation,
    channel_norm_gain,
    taps,
    proj_weight,
    gate_weight,
    up_weight,
    down_weight,
):
    experts = lax.axis_size("sp")
    groups = lax.axis_size("tp")
    tok_rows, model_width = cotangent.shape
    capacity = groups * max(1, 4 * tok_rows // (experts * groups))
    slot_span = capacity // groups
    slot_start = lax.axis_index("tp") * slot_span
    dispatch, slot_weight = route_table(
        expert_ids, route_weight, slot_start, slot_span, capacity, experts
    )
    sent_rows = jnp.dot(dispatch, mixer_out, preferred_element_type=jnp.float32).astype(
        jnp.bfloat16
    )
    sent_grad = (
        slot_weight[:, None] * jnp.dot(dispatch, cotangent, preferred_element_type=jnp.float32)
    ).astype(jnp.bfloat16)
    sent_rows = sent_rows.reshape(experts, slot_span, model_width)
    sent_grad = sent_grad.reshape(experts, slot_span, model_width)
    normalized_input = saved_normalized.astype(jnp.float32)
    normalized_values = normalized_input * channel_norm_gain[None, :]
    gate_sig = jax.nn.sigmoid(normalized_values)
    act_conv = (normalized_values * gate_sig).astype(jnp.bfloat16)
    act_conv, sent_rows = lax.optimization_barrier((act_conv, sent_rows))
    every_act = lax.all_gather(act_conv, "sp", axis=0, tiled=True)
    routed_rows, routed_grad = dispatch_blocks(sent_rows, sent_grad, groups)
    full_table, unused_weight = route_table(
        expert_ids, route_weight, 0, capacity, capacity, experts
    )
    routed_rows = routed_rows.reshape(-1, model_width)
    routed_grad = routed_grad.reshape(-1, model_width)
    w_first = gate_weight[0]
    w_third = up_weight[0]
    w_second = down_weight[0]
    contract_last = (((1,), (1,)), ((), ()))
    contract_first = (((0,), (0,)), ((), ()))
    hidden_gate = jnp.dot(routed_rows, w_first, preferred_element_type=jnp.float32)
    hidden_up = jnp.dot(routed_rows, w_third, preferred_element_type=jnp.float32)
    sigma = jax.nn.sigmoid(hidden_gate)
    swish = hidden_gate * sigma
    activ = (swish * hidden_up).astype(jnp.bfloat16)
    grad_second = lax.dot_general(
        activ, routed_grad, contract_first, preferred_element_type=jnp.float32
    ).astype(jnp.bfloat16)
    grad_activ = lax.dot_general(
        routed_grad, w_second, contract_last, preferred_element_type=jnp.float32
    )
    grad_gpre = (grad_activ * hidden_up * sigma * (1.0 + hidden_gate * (1.0 - sigma))).astype(
        jnp.bfloat16
    )
    grad_upre = (grad_activ * swish).astype(jnp.bfloat16)
    grad_first = lax.dot_general(
        routed_rows, grad_gpre, contract_first, preferred_element_type=jnp.float32
    ).astype(jnp.bfloat16)
    grad_third = lax.dot_general(
        routed_rows, grad_upre, contract_first, preferred_element_type=jnp.float32
    ).astype(jnp.bfloat16)
    partial_value = lax.dot_general(
        grad_gpre, w_first, contract_last, preferred_element_type=jnp.float32
    ) + lax.dot_general(grad_upre, w_third, contract_last, preferred_element_type=jnp.float32)
    share = model_width // groups
    partial_groups = jnp.transpose(
        partial_value.astype(jnp.bfloat16).reshape(-1, groups, share), (1, 0, 2)
    )
    every_act, partial_groups = lax.optimization_barrier((every_act, partial_groups))
    home_rows = home_blocks(partial_groups.reshape(groups, experts, capacity, share))
    returned = lax.dot_general(
        full_table,
        home_rows.reshape(-1, share),
        contract_first,
        preferred_element_type=jnp.float32,
    )
    own_cotangent = lax.dynamic_slice_in_dim(
        cotangent, lax.axis_index("tp") * share, share, axis=1
    )
    mixer_share = (own_cotangent.astype(jnp.float32) + returned).astype(jnp.bfloat16)
    mixer_grad = lax.all_gather(mixer_share, "tp", axis=1, tiled=True)
    width_share = model_width // experts
    sent_columns = jnp.transpose(
        mixer_grad.reshape(tok_rows, experts, width_share), (1, 0, 2)
    )
    every_grad = lax.all_to_all(
        sent_columns, "sp", split_axis=0, concat_axis=0, tiled=True
    ).reshape(-1, width_share)
    grad_proj = lax.dot_general(
        every_grad, every_act, contract_first, preferred_element_type=jnp.float32
    )
    grad_act = lax.dot_general(
        mixer_grad, proj_weight, contract_last, preferred_element_type=jnp.float32
    )
    norm_output_gradient = (
        grad_act
        * gate_sig
        * (1.0 + normalized_values * (1.0 - gate_sig))
        * channel_norm_gain[None, :]
    )
    reduced_totals = lax.psum(
        (
            jnp.sum(norm_output_gradient, axis=1),
            jnp.sum(norm_output_gradient * normalized_input, axis=1),
        ),
        "tp",
    )
    channel_count = saved_normalized.shape[1] * groups
    conv_output_gradient = inverse_deviation[:, None] * (
        norm_output_gradient
        - reduced_totals[0][:, None] / channel_count
        - normalized_input * (reduced_totals[1][:, None] / channel_count)
    )
    reach = taps.shape[0] - 1
    beyond = from_behind(conv_output_gradient[:reach], "sp", -1)
    extended = jnp.concatenate([conv_output_gradient, beyond], axis=0)
    result = jnp.zeros_like(conv_output_gradient)
    for tap_index in range(taps.shape[0]):
        result = result + taps[tap_index][None, :] * extended[tap_index : tap_index + tok_rows]
    return (
        result.astype(jnp.bfloat16),
        grad_proj,
        grad_first[None],
        grad_third[None],
        grad_second[None],
    )


def solution(mesh):
    return jax.shard_map(
        shards,
        mesh=mesh,
        in_specs=(
            P("sp", None),
            P("sp", None),
            P("sp", None),
            P("sp", None),
            P("sp", "tp"),
            P("sp"),
            P("tp"),
            P(None, "tp"),
            P("tp", None),
            P("sp", None, "tp"),
            P("sp", None, "tp"),
            P("sp", "tp", None),
        ),
        out_specs=(
            P("sp", "tp"),
            P("sp", "tp"),
            P("sp", None, "tp"),
            P("sp", None, "tp"),
            P("sp", "tp", None),
        ),
        check_vma=False,
    )
```
